32 devices in a mesh: sp: 8 (over z, y), tp: 4 (over x, core).
Axes of the slice: x: 2, y: 2, z: 4, core: 2. Of those that a mesh axis runs over, the one named last changes fastest.
Arguments:
- queries: bfloat16 [2048, 2048], P('sp', 'tp'), may hold values from -16 to 16
- key_value_pairs: bfloat16 [2048, 512], P('sp', 'tp'), may hold values from -16 to 16
- forget_gate_total: float32 [2048, 32], P('sp', 'tp'), may hold values from -2048 to 0, as said below
- residual_in: bfloat16 [2048, 2048], P(('sp', 'tp')), may hold values from -12 to 12
- out_weight: bfloat16 [2048, 2048], P('tp'), may hold values from -0.25 to 0.25
- norm_gain: float32 [2048], replicated, may hold values from 0.1 to 1.9
- routes: int32 [2048, 2], P(('sp', 'tp')), may hold values from 0 to 7, all different within a row; in each aligned block of 64 rows (0 to 63, 64 to 127, ...) at most 24 rows name the same one
- route_weight: float32 [2048, 2], P(('sp', 'tp')), may hold values from 0.2 to 1
- expert_gate: bfloat16 [8, 2048, 3072], P('sp', None, 'tp'), may hold values from -0.125 to 0.125
- expert_up: bfloat16 [8, 2048, 3072], P('sp', None, 'tp'), may hold values from -0.125 to 0.125
- expert_down: bfloat16 [8, 3072, 2048], P('sp', 'tp'), may hold values from -0.109375 to 0.109375
Outputs:
- layer_out: bfloat16 [2048, 2048], P(('sp', 'tp'))
The draws below stay inside these ranges and needn't reach their ends.
Inputs may be any that keep to these rules, and one draw needn't show every extreme that they name: `routes`: each row names 2 different experts; among the rows of one device no expert is named more than 24 times, and in every draw some device names some expert exactly 24 times. `forget_gate_total`: along the positions, each head's values never rise.
All inputs are finite; a program needn't handle non-finite values.
Results may differ from the reference program's by a relative error of at most 0.011.
Values may be sent and summed in bfloat16 or wider, within the bound.
A program may use at most 64 MiB of HBM per device.

```python
import math
import jax
import jax.numpy as jnp
import numpy as np
from jax import lax

D = 2048
QUERY_HEADS = 32
KEY_VALUE_HEADS = 4
HEAD_SIZE = 64
FF = 3072
TOP = 2
TOK_DEV = 256
SEQUENCE_TOKENS = 2048
ROWS_DEV = 64
EXPERTS = 8
CAPACITY = 24
N_SP = 8
N_TP = 4


def draw_queries(key, part):
    array_shape = (SEQUENCE_TOKENS, QUERY_HEADS * HEAD_SIZE)
    base = jax.random.normal(jax.random.fold_in(key, 1), array_shape, jnp.float32)
    return jnp.clip(1.4 * base, -5.6, 5.6).astype(jnp.bfloat16)


def draw_key_value_pairs(key, part):
    array_shape = (SEQUENCE_TOKENS, KEY_VALUE_HEADS, HEAD_SIZE)
    key_portion = jnp.clip(1.4 * jax.random.normal(jax.random.fold_in(key, 2), array_shape, jnp.float32), -5.6, 5.6)
    value_portion = jnp.clip(jax.random.normal(jax.random.fold_in(key, 3), array_shape, jnp.float32), -4.0, 4.0)
    return jnp.concatenate([key_portion, value_portion], axis=2).reshape(SEQUENCE_TOKENS, KEY_VALUE_HEADS * 2 * HEAD_SIZE).astype(jnp.bfloat16)


def draw_forget_gate_total(key, part):
    order = jax.random.permutation(jax.random.fold_in(key, 21), QUERY_HEADS)
    fast = order < QUERY_HEADS // 2
    slow_total = jnp.exp(jax.random.uniform(jax.random.fold_in(key, 22), (QUERY_HEADS,), jnp.float32, math.log(0.2), math.log(0.8)))
    fast_rate = jnp.exp(jax.random.uniform(jax.random.fold_in(key, 23), (QUERY_HEADS,), jnp.float32, math.log(0.03), math.log(0.1)))
    rate = jnp.where(fast, fast_rate, slow_total / SEQUENCE_TOKENS)
    blocks = SEQUENCE_TOKENS // TOK_DEV
    block_factor = jnp.exp(jax.random.uniform(jax.random.fold_in(key, 24), (blocks, QUERY_HEADS), jnp.float32, math.log(0.5), math.log(2.0)))
    rough = jax.random.uniform(jax.random.fold_in(key, 25), (SEQUENCE_TOKENS, QUERY_HEADS), jnp.float32, 0.3, 1.7)
    loop_steps = rate[None, :] * jnp.repeat(block_factor, TOK_DEV, axis=0) * rough
    segment_begin = jax.random.randint(jax.random.fold_in(key, 26), (2,), 0, SEQUENCE_TOKENS)
    segment_length = jax.random.uniform(jax.random.fold_in(key, 27), (2, QUERY_HEADS), jnp.float32, 0.2, 0.4)
    segment_list = jnp.zeros((SEQUENCE_TOKENS, QUERY_HEADS), jnp.float32).at[segment_begin].add(-jnp.log(1.0 - segment_length))
    return -jnp.cumsum(loop_steps + segment_list, axis=0)


def draw_residual_in(key, part):
    base = jax.random.normal(jax.random.fold_in(key, 31), (SEQUENCE_TOKENS, D), jnp.float32)
    return jnp.clip(base, -6.0, 6.0).astype(jnp.bfloat16)


def levels(own_key, extent, split, least, top_value):
    def one(axis_at, shards_of):
        steps = jax.random.uniform(jax.random.fold_in(jax.random.fold_in(own_key, 6), axis_at), (shards_of,), jnp.float32, least / len(split), top_value / len(split))
        return jnp.repeat(jnp.exp(steps), extent[axis_at] // shards_of).reshape((-1,) + (1,) * (len(extent) - axis_at - 1))

    level = one(*split[0])
    for cut in split[1:]:
        level = level * one(*cut)
    return level


def assign_block(stream_key, own, number, rows, count, top, most, lean):
    order = jax.random.permutation(stream_key, count)
    packed, ordinary = shares(count, rows * top, most, lean, True), shares(count, rows * top, most, lean, False)
    places = jnp.arange(count)

    def named(sizes, rotation):
        used = int((sizes > 0).sum())
        fixed = max(1, used // 4)
        moved = fixed + (places - fixed + rotation * (used - fixed)) % max(1, count - fixed)
        return jnp.zeros((count,), jnp.int32).at[order[jnp.where(places < fixed, places, moved)]].set(jnp.asarray(sizes, jnp.int32))

    sizes = jnp.where(number % 4 == 0, named(packed, number // 4), named(ordinary, number - number // 4 - 1))
    mixed = jax.random.permutation(jax.random.fold_in(own, 3), count)
    source_of, receiver = mixed[0:count // 2 * 2:2], mixed[1:count // 2 * 2:2]
    slack = jnp.minimum(sizes[source_of] - 1, most - sizes[receiver]) // 2
    slack = jnp.where((source_of == order[0]) | (receiver == order[0]) | (sizes[receiver] == 0), 0, jnp.maximum(slack, 0))
    moved = jax.random.randint(jax.random.fold_in(own, 4), (count // 2,), 0, 1 << 20) % (slack + 1)
    sizes = sizes.at[source_of].add(-moved).at[receiver].add(moved)
    members = jnp.searchsorted(jnp.cumsum(sizes), jnp.arange(rows * top), side="right").astype(jnp.int32)
    grid = members.reshape(top, rows).T
    grid = grid[jax.random.permutation(jax.random.fold_in(own, 1), rows)]
    rotation = jax.random.randint(jax.random.fold_in(own, 2), (rows, 1), 0, top)
    return jnp.take_along_axis(grid, (jnp.arange(top)[None, :] + rotation) % top, axis=1)


def shares(count, total, most, slope, full):
    weights = [(1 << 20) // math.isqrt(rank ** slope) + 1 for rank in range(1, count + 1)]
    largest = most if full else min(most, max(-(-total // count), total * weights[0] // sum(weights)))
    least = 1 if total - largest >= count - 1 else 0
    holding, rest = [largest] + [least] * (count - 1), total - largest - least * (count - 1)
    while rest > 0:
        candidates = [i for i in range(1, count) if holding[i] < largest] or [i for i in range(1, count) if holding[i] < most]
        pool, left = sum([weights[i] for i in candidates]), rest
        for i in candidates:
            addition = min(most - holding[i], max(1, left * weights[i] // pool), rest)
            holding[i] = holding[i] + addition
            rest = rest - addition
    return np.array(holding)


def centred(own_key, shape, width, reach, split=(), held_as=jnp.bfloat16):
    values = jax.random.normal(own_key, shape, jnp.float32) * width
    if len(split) > 0:
        values = levels(own_key, shape, split, -0.22, 0.18) * values
    return jnp.clip(values, min=-reach, max=reach).astype(held_as)


def setup_inputs(seed: int = 0) -> dict:
    key_list = jax.random.split(jax.random.key(seed), 12)
    queries = draw_queries(jax.random.fold_in(key_list[11], 71), 0)
    key_value_pairs = draw_key_value_pairs(jax.random.fold_in(key_list[11], 71), 0)
    forget_gate_total = draw_forget_gate_total(jax.random.fold_in(key_list[11], 71), 0)
    residual_in = draw_residual_in(jax.random.fold_in(key_list[11], 71), 0)
    out_weight = centred(key_list[4], (QUERY_HEADS * HEAD_SIZE, D), (QUERY_HEADS * HEAD_SIZE // 4) ** -0.5, 0.25, ((0, 4),))
    norm_gain = jnp.clip(1.0 + 0.18 * jax.random.normal(key_list[5], (D,), jnp.float32), 0.1, 1.9)
    routes_keys = jax.random.split(jax.random.fold_in(key_list[6], 1), SEQUENCE_TOKENS // ROWS_DEV)
    routes_turns = jax.random.permutation(jax.random.fold_in(key_list[6], 3), SEQUENCE_TOKENS // ROWS_DEV)
    routes = jax.vmap(lambda own, number: assign_block(jax.random.fold_in(key_list[6], 2), own, number, ROWS_DEV, EXPERTS, TOP, CAPACITY, 2))(routes_keys, routes_turns).reshape((SEQUENCE_TOKENS, TOP))
    route_weight = jnp.clip(0.2 + 0.8 * jax.random.uniform(key_list[7], (SEQUENCE_TOKENS, TOP), jnp.float32) ** levels(key_list[7], (SEQUENCE_TOKENS, TOP), ((0, 32),), -0.2, 0.2), 0.2, 1.0)
    expert_gate = centred(key_list[8], (EXPERTS, D, FF), D ** -0.5, 0.125, ((0, 8), (2, 4)))
    expert_up = centred(key_list[9], (EXPERTS, D, FF), D ** -0.5, 0.125, ((0, 8), (2, 4)))
    expert_down = centred(key_list[10], (EXPERTS, FF, D), FF ** -0.5, 0.109375, ((0, 8), (1, 4)))
    return {"queries": queries, "key_value_pairs": key_value_pairs, "forget_gate_total": forget_gate_total, "residual_in": residual_in, "out_weight": out_weight, "norm_gain": norm_gain, "routes": routes, "route_weight": route_weight, "expert_gate": expert_gate, "expert_up": expert_up, "expert_down": expert_down}


NEG_FILL = -1e+30
NORM_EPS = 1e-06

def round_half(values):
    return lax.optimization_barrier(values.astype(jnp.bfloat16)).astype(jnp.float32)

def attention(queries, key_value_pairs, forget_gate_total):
    token_total = queries.shape[0]
    queries_per_group = QUERY_HEADS // KEY_VALUE_HEADS
    score_scale = HEAD_SIZE ** (-0.5)
    grouped_queries = queries.reshape(token_total, KEY_VALUE_HEADS, queries_per_group, HEAD_SIZE)
    key_value_head_list = key_value_pairs.reshape(token_total, KEY_VALUE_HEADS, 2 * HEAD_SIZE)
    key_rows = key_value_head_list[:, :, :HEAD_SIZE].astype(jnp.float32)
    value_rows = key_value_head_list[:, :, HEAD_SIZE:].astype(jnp.float32)
    gate_row_slice = forget_gate_total.reshape(token_total, KEY_VALUE_HEADS, queries_per_group)
    key_gate = jnp.transpose(gate_row_slice, (1, 2, 0))
    key_pos = jnp.arange(token_total, dtype=jnp.int32)
    query_count = math.gcd(token_total, 128)

    def query_block(block_index):
        first_row = block_index * query_count
        query_rows = lax.dynamic_slice_in_dim(grouped_queries, first_row, query_count, 0).astype(jnp.float32)
        query_gate = lax.dynamic_slice_in_dim(gate_row_slice, first_row, query_count, 0)
        scores = jnp.einsum('tkgd,skd->ktgs', query_rows, key_rows) * score_scale
        scores = scores + jnp.transpose(query_gate, (1, 0, 2))[..., None] - key_gate[:, None, :, :]
        query_pos = first_row + jnp.arange(query_count, dtype=jnp.int32)
        scores = jnp.where(key_pos[None, None, None, :] <= query_pos[None, :, None, None], scores, NEG_FILL)
        row_max = lax.optimization_barrier(jnp.max(scores, axis=3, keepdims=True))
        weights = jnp.exp(scores - row_max)
        totals = lax.optimization_barrier(jnp.sum(weights, axis=3))
        numer = jnp.einsum('ktgs,skd->ktgd', round_half(weights), value_rows)
        result = numer / totals[..., None]
        return jnp.transpose(result, (1, 0, 2, 3)).reshape(query_count, QUERY_HEADS * HEAD_SIZE).astype(jnp.bfloat16)
    blocks = lax.map(query_block, jnp.arange(token_total // query_count, dtype=jnp.int32))
    return blocks.reshape(token_total, QUERY_HEADS * HEAD_SIZE)

def apply_experts(normed, routes, route_weight, expert_gate, expert_up, expert_down):
    token_total = normed.shape[0]
    chosen = routes.reshape(-1)
    flat_weight = route_weight.reshape(-1)
    slot_count = chosen.shape[0]
    most_rows = N_SP * N_TP * CAPACITY
    unit_width = FF // N_TP

    def one_expert(totals, inputs):
        expert_index, w_gate, w_up, w_down = inputs
        picked = jnp.nonzero(chosen == expert_index, size=most_rows, fill_value=slot_count)[0].astype(jnp.int32)
        usable = picked < slot_count
        safe_slot = jnp.minimum(picked, slot_count - 1)
        token_rows = safe_slot // TOP
        input_rows = normed[token_rows]
        expert_sum = jnp.zeros((most_rows, D), jnp.float32)
        for column in range(N_TP):
            col_band = slice(column * unit_width, (column + 1) * unit_width)
            gate_value = jnp.dot(input_rows, w_gate[:, col_band], preferred_element_type=jnp.float32)
            up_value = jnp.dot(input_rows, w_up[:, col_band], preferred_element_type=jnp.float32)
            hidden_rows = (jax.nn.silu(gate_value) * up_value).astype(jnp.bfloat16)
            expert_sum = expert_sum + round_half(jnp.dot(hidden_rows, w_down[col_band, :], preferred_element_type=jnp.float32))
        weighted = jnp.where(usable, flat_weight[safe_slot], 0.0)[:, None] * round_half(expert_sum)
        return (totals.at[token_rows].add(weighted), None)
    start_totals = jnp.zeros((token_total, D), jnp.float32)
    totals, _ = lax.scan(one_expert, start_totals, (jnp.arange(EXPERTS, dtype=jnp.int32), expert_gate, expert_up, expert_down))
    return totals

def reference(queries, key_value_pairs, forget_gate_total, residual_in, out_weight, norm_gain, routes, route_weight, expert_gate, expert_up, expert_down):
    attended = attention(queries, key_value_pairs, forget_gate_total)
    head_width = QUERY_HEADS * HEAD_SIZE // N_TP
    mixed_rows = jnp.zeros((attended.shape[0], D), jnp.float32)
    for column in range(N_TP):
        col_band = slice(column * head_width, (column + 1) * head_width)
        mixed_rows = mixed_rows + round_half(jnp.dot(attended[:, col_band], out_weight[col_band, :], preferred_element_type=jnp.float32))
    hidden_state = residual_in.astype(jnp.float32) + mixed_rows
    normed = (hidden_state * lax.rsqrt(lax.optimization_barrier(jnp.mean(hidden_state * hidden_state, axis=1, keepdims=True)) + NORM_EPS) * norm_gain).astype(jnp.bfloat16)
    combined = apply_experts(normed, routes, route_weight, expert_gate, expert_up, expert_down)
    return (hidden_state + combined).astype(jnp.bfloat16)
```

```python
import functools

import jax
import jax.numpy as jnp
from jax import lax
from jax.experimental import pallas as pl
from jax.experimental.pallas import tpu as pltpu
from jax.sharding import PartitionSpec as P

HEAD_SIZE = 64
NEG_FILL = -1e30
NORM_EPS = 1e-06
OUTER = 2
MESH = pl.DeviceIdType.MESH
F32 = jnp.float32
BF16 = jnp.bfloat16


def greet(peers_sp, sp_count, sp, tp, tp_peers):
    barrier = pltpu.get_barrier_semaphore()

    def signal(step, carry):
        pl.semaphore_signal(
            barrier, inc=1, device_id=(lax.rem(sp + step, sp_count), tp), device_id_type=MESH
        )
        return carry

    lax.fori_loop(1, sp_count, signal, 0)
    for peer in tp_peers:
        pl.semaphore_signal(barrier, inc=1, device_id=(sp, peer), device_id_type=MESH)
    return lambda: pl.semaphore_wait(barrier, sp_count - 1 + len(tp_peers))


def remote(src, dst, send, recv, device):
    return pltpu.make_async_remote_copy(
        src_ref=src,
        dst_ref=dst,
        send_sem=send,
        recv_sem=recv,
        device_id=device,
        device_id_type=MESH,
    )


def tp_places(tp, tp_count):
    inner = tp_count // OUTER
    a, c = tp // inner, lax.rem(tp, inner)
    mates = [a * inner + lax.rem(c + k, inner) for k in range(1, inner)]
    across = (1 - a) * inner + c
    return inner, a, c, mates, across


def mix_kernel(
    sp_count,
    tp_count,
    q_ref,
    kv_ref,
    gate_ref,
    gate_rows_ref,
    resid_ref,
    gain_ref,
    wout_hbm,
    hidden_ref,
    normed_ref,
    kv_all,
    gate_all,
    qm_ref,
    max_ref,
    acc_ref,
    att_ref,
    wout,
    mate_out,
    mate_in,
    own_sum,
    far_out,
    far_in,
    w_sem,
    kv_send,
    kv_recv,
    gate_send,
    gate_recv,
    mate_send,
    mate_recv,
    far_send,
    far_recv,
):
    sp, tp = lax.axis_index("sp"), lax.axis_index("tp")
    inner, a, c, mates, across = tp_places(tp, tp_count)
    rows, width = q_ref.shape
    heads = width // HEAD_SIZE
    pair = 2 * HEAD_SIZE
    groups = kv_ref.shape[1] // pair
    per_group = heads // groups
    own = rows // tp_count
    ready = greet(None, sp_count, sp, tp, mates + [across])
    load = pltpu.make_async_copy(wout_hbm, wout, w_sem)
    load.start()

    low = lax.broadcasted_iota(jnp.int32, (rows, pair), 1) < HEAD_SIZE
    for h in range(heads):
        base = (h // 2) * pair
        block = q_ref[:, base : base + pair].astype(F32) * (HEAD_SIZE**-0.5)
        keep = low if h % 2 == 0 else jnp.logical_not(low)
        qm_ref[h] = jnp.where(keep, block, 0.0).astype(BF16)
    ready()

    def kv_copy(source, target):
        return remote(
            kv_ref, kv_all.at[source], kv_send.at[target], kv_recv.at[source], (target, tp)
        )

    def gate_copy(source, target):
        return remote(
            gate_rows_ref,
            gate_all.at[source],
            gate_send.at[target],
            gate_recv.at[source],
            (target, tp),
        )

    def send(target, carry):
        kv_copy(sp, target).start()
        gate_copy(sp, target).start()
        return carry

    lax.fori_loop(sp + 1, sp_count, send, 0)

    def attend(kv, gates, first):
        causal = None
        if first:
            causal = lax.broadcasted_iota(jnp.int32, (rows, rows), 1) <= lax.broadcasted_iota(
                jnp.int32, (rows, rows), 0
            )
        for g in range(groups):
            both = kv[:, g * pair : (g + 1) * pair].astype(F32)
            swapped = pltpu.roll(both, HEAD_SIZE, 1)
            keys = jnp.where(low, both, swapped).astype(BF16)
            values = (
                jnp.where(low, swapped, 1.0).astype(BF16),
                jnp.where(low, 1.0, both).astype(BF16),
            )
            for h in range(g * per_group, (g + 1) * per_group):
                scores = lax.dot_general(
                    qm_ref[h], keys, (((1,), (1,)), ((), ())), preferred_element_type=F32
                )
                scores = scores + gate_ref[:, h : h + 1] - gates[h : h + 1, :]
                if first:
                    scores = jnp.where(causal, scores, NEG_FILL)
                top = jnp.max(scores, axis=1, keepdims=True)
                if not first:
                    old = max_ref[h]
                    top = jnp.maximum(old, top)
                weights = jnp.exp(scores - top).astype(BF16)
                block_sum = jnp.dot(weights, values[h % 2], preferred_element_type=F32)
                if first:
                    acc_ref[h] = block_sum
                else:
                    acc_ref[h] = acc_ref[h] * jnp.exp(old - top) + block_sum
                max_ref[h] = top

    attend(kv_ref[...], gate_rows_ref[...], True)

    def earlier(step, carry):
        source = sp - step
        kv_copy(source, sp).wait_recv()
        gate_copy(source, sp).wait_recv()
        attend(kv_all[source], gate_all[source], False)
        return carry

    lax.fori_loop(1, sp + 1, earlier, 0)

    for h in range(0, heads, 2):
        even, odd = acc_ref[h], acc_ref[h + 1]
        even = even / pltpu.roll(even, HEAD_SIZE, 1)
        odd = odd / pltpu.roll(odd, HEAD_SIZE, 1)
        att_ref[:, (h // 2) * pair : (h // 2 + 1) * pair] = jnp.where(low, even, odd).astype(BF16)

    load.wait()

    def product(column):
        parts = [
            att_ref[pl.ds(pl.multiple_of((o * inner + column) * own, own), own), :]
            for o in range(OUTER)
        ]
        return jnp.dot(jnp.concatenate(parts, axis=0), wout[...], preferred_element_type=F32)

    mate_copies = []
    for k, mate in enumerate(mates):
        mate_out[k] = product(lax.rem(mate, inner)).astype(BF16)
        copy = remote(
            mate_out.at[k], mate_in.at[k], mate_send.at[k], mate_recv.at[k], (sp, mate)
        )
        copy.start()
        mate_copies.append(copy)
    own_sum[...] = product(c).reshape(OUTER, own, own_sum.shape[2])
    for k, copy in enumerate(mate_copies):
        copy.wait_recv()
        own_sum[...] += mate_in[k].astype(F32).reshape(own_sum.shape)
    far_out[...] = own_sum[1 - a].astype(BF16)
    far = remote(far_out, far_in, far_send, far_recv, (sp, across))
    far.start()
    far.wait_recv()
    hidden = resid_ref[...].astype(F32) + own_sum[a] + far_in[...].astype(F32)
    hidden_ref[...] = hidden
    scale = lax.rsqrt(jnp.mean(hidden * hidden, axis=1, keepdims=True) + NORM_EPS)
    normed_ref[...] = (hidden * scale * gain_ref[...]).astype(BF16)
    far.wait_send()
    for copy in mate_copies:
        copy.wait_send()

    def finish(target, carry):
        kv_copy(sp, target).wait_send()
        gate_copy(sp, target).wait_send()
        return carry

    lax.fori_loop(sp + 1, sp_count, finish, 0)


def expert_kernel(
    sp_count,
    tp_count,
    cap,
    normed_ref,
    hidden_ref,
    slot_cols_ref,
    slot_rows_ref,
    weight_ref,
    gate_hbm,
    up_hbm,
    down_hbm,
    out_ref,
    outgoing,
    inbox,
    w_gate,
    w_up,
    w_down,
    partial,
    mate_in,
    chip_sum,
    far_in,
    final,
    back,
    w_sem,
    own_sem,
    s1,
    r1,
    s2,
    r2,
    s3,
    r3,
    s4,
    r4,
    s5,
    r5,
    s6,
    r6,
    s7,
    r7,
):
    sp, tp = lax.axis_index("sp"), lax.axis_index("tp")
    inner, a, c, mates, across = tp_places(tp, tp_count)
    own, width = normed_ref.shape
    slots = sp_count * cap
    ready = greet(None, sp_count, sp, tp, mates + [across])
    loads = [
        pltpu.make_async_copy(src.at[0], dst, w_sem.at[i])
        for i, (src, dst) in enumerate(
            ((gate_hbm, w_gate), (up_hbm, w_up), (down_hbm, w_down))
        )
    ]
    for load in loads:
        load.start()
    slot_at = lax.broadcasted_iota(jnp.int32, (slots, own), 0)
    chosen = slot_rows_ref[...]
    pick = jnp.zeros((slots, own), F32)
    for k in range(chosen.shape[0]):
        pick = pick + jnp.where(slot_at == chosen[k : k + 1, :], 1.0, 0.0)
    sent = jnp.dot(pick.astype(BF16), normed_ref[...], preferred_element_type=F32)
    outgoing[...] = sent.reshape(sp_count, cap, width).astype(BF16)
    ready()

    def at(step):
        return lax.rem(sp + step, sp_count)

    def before(step):
        return lax.rem(sp + sp_count - step, sp_count)

    def to_expert(target, source):
        return remote(
            outgoing.at[target], inbox.at[source, c, a], s1.at[target], r1.at[source], (target, tp)
        )

    def to_across(source):
        return remote(
            inbox.at[source, c, a], inbox.at[source, c, a], s2.at[source], r2.at[source], (sp, across)
        )

    def from_across(source):
        return remote(
            inbox.at[source, c, a],
            inbox.at[source, c, 1 - a],
            s2.at[source],
            r2.at[source],
            (sp, across),
        )

    def to_mate(k, source, o, send, recv):
        return remote(
            inbox.at[source, c, o], inbox.at[source, c, o], send.at[k, source], recv.at[k, source],
            (sp, mates[k]),
        )

    def from_mate(k, source, o, send, recv):
        sender = lax.rem(c + inner - (k + 1), inner)
        return remote(
            inbox.at[source, c, o],
            inbox.at[source, sender, o],
            send.at[k, source],
            recv.at[k, source],
            (sp, mates[k]),
        )

    def start_one(step, carry):
        to_expert(at(step), sp).start()
        return carry

    lax.fori_loop(1, sp_count, start_one, 0)
    keep = pltpu.make_async_copy(outgoing.at[sp], inbox.at[sp, c, a], own_sem)
    keep.start()
    keep.wait()

    def forward(source):
        to_across(source).start()
        for k in range(len(mates)):
            to_mate(k, source, a, s3, r3).start()

    def forward_across(source):
        from_across(source).wait_recv()
        for k in range(len(mates)):
            to_mate(k, source, 1 - a, s4, r4).start()

    forward(sp)

    def dispatch(step, carry):
        source = before(step)
        to_expert(sp, source).wait_recv()
        forward(source)
        forward_across(before(step - 1))
        return carry

    lax.fori_loop(1, sp_count, dispatch, 0)
    forward_across(before(sp_count - 1))
    for load in loads:
        load.wait()

    def compute(step):
        source = before(step)
        for k in range(len(mates)):
            from_mate(k, source, a, s3, r3).wait_recv()
            from_mate(k, source, 1 - a, s4, r4).wait_recv()

    def load_rows(source):
        return inbox[source].astype(F32).reshape(tp_count * cap, width).astype(BF16)

    def send_mate(k, source):
        return remote(
            partial.at[source, lax.rem(mates[k], inner)],
            mate_in.at[k, source],
            s5.at[k, source],
            r5.at[k, source],
            (sp, mates[k]),
        )

    def send_far(source):
        return remote(
            chip_sum.at[source, 1 - a], far_in.at[source], s6.at[source], r6.at[source], (sp, across)
        )

    def send_back(target, source):
        return remote(
            final.at[target], back.at[source], s7.at[target], r7.at[source], (target, tp)
        )

    batch = 2 if sp_count % 2 == 0 else 1
    steps = sp_count // batch

    def ffn(i):
        for b in range(batch):
            compute(i * batch + b)
        x = jnp.concatenate([load_rows(before(i * batch + b)) for b in range(batch)], axis=0)
        gate = jnp.dot(x, w_gate[...], preferred_element_type=F32)
        up = jnp.dot(x, w_up[...], preferred_element_type=F32)
        hidden = (gate / (1.0 + jnp.exp(-gate)) * up).astype(BF16)
        y = jnp.dot(hidden, w_down[...], preferred_element_type=F32)
        y = y.reshape(batch, inner, OUTER, cap, width).astype(BF16)
        for b in range(batch):
            source = before(i * batch + b)
            partial[source] = y[b]
            for k in range(len(mates)):
                send_mate(k, source).start()

    def chip(i):
        for b in range(batch):
            source = before(i * batch + b)
            total = partial[source, c].astype(F32)
            for k in range(len(mates)):
                send_mate(k, source).wait_recv()
                total = total + mate_in[k, source].astype(F32)
            chip_sum[source] = total.astype(BF16)
            send_far(source).start()

    def give_back(i):
        for b in range(batch):
            step = i * batch + b
            source = before(step)
            send_far(source).wait_recv()
            total = chip_sum[source, a].astype(F32) + far_in[source].astype(F32)
            final[source] = total.astype(BF16)

            @pl.when(step > 0)
            def _():
                send_back(source, sp).start()

    def pipeline(i, carry):
        ffn(i)

        @pl.when(i >= 1)
        def _():
            chip(i - 1)

        @pl.when(i >= 2)
        def _():
            give_back(i - 2)

        return carry

    lax.fori_loop(0, steps, pipeline, 0)
    chip(steps - 1)
    if steps >= 2:
        give_back(steps - 2)
    give_back(steps - 1)
    back[sp] = final[sp]

    slot_of = lax.broadcasted_iota(jnp.int32, (own, slots), 1)
    share = jnp.zeros((own, slots), F32)
    for k in range(slot_cols_ref.shape[1]):
        share = share + jnp.where(
            slot_of == slot_cols_ref[:, k : k + 1], weight_ref[:, k : k + 1], 0.0
        )
    high = share.astype(BF16)
    rest = share - high.astype(F32)
    middle = rest.astype(BF16)
    least = (rest - middle.astype(F32)).astype(BF16)

    def arrive(step, carry):
        send_back(sp, at(step)).wait_recv()
        return carry

    lax.fori_loop(1, sp_count, arrive, 0)
    results = back[...].astype(F32).reshape(slots, width).astype(BF16)
    combined = hidden_ref[...]
    for piece in (high, middle, least):
        combined = combined + jnp.dot(piece, results, preferred_element_type=F32)
    out_ref[...] = combined.astype(BF16)

    def finish(step, carry):
        source = at(step)
        to_across(source).wait_send()
        send_far(source).wait_send()
        for k in range(len(mates)):
            to_mate(k, source, a, s3, r3).wait_send()
            to_mate(k, source, 1 - a, s4, r4).wait_send()
            send_mate(k, source).wait_send()

        @pl.when(step > 0)
        def _():
            to_expert(source, sp).wait_send()
            send_back(source, sp).wait_send()

        return carry

    lax.fori_loop(0, sp_count, finish, 0)


def local(
    queries,
    key_value_pairs,
    forget_gate_total,
    residual_in,
    out_weight,
    norm_gain,
    routes,
    route_weight,
    expert_gate,
    expert_up,
    expert_down,
):
    sp_count = lax.axis_size("sp")
    tp_count = lax.axis_size("tp")
    rows, q_width = queries.shape
    heads = q_width // HEAD_SIZE
    own, width = residual_in.shape
    inner = tp_count // OUTER
    vmem = pl.BlockSpec(memory_space=pltpu.VMEM)
    hbm = pl.BlockSpec(memory_space=pl.ANY)
    dma = pltpu.SemaphoreType.DMA
    hidden, normed = pl.pallas_call(
        functools.partial(mix_kernel, sp_count, tp_count),
        out_shape=(
            jax.ShapeDtypeStruct((own, width), F32),
            jax.ShapeDtypeStruct((own, width), BF16),
        ),
        in_specs=[vmem] * 6 + [hbm],
        out_specs=(vmem, vmem),
        scratch_shapes=[
            pltpu.VMEM((sp_count, rows, key_value_pairs.shape[1]), BF16),
            pltpu.VMEM((sp_count, heads, rows), F32),
            pltpu.VMEM((heads, rows, 2 * HEAD_SIZE), BF16),
            pltpu.VMEM((heads, rows, 1), F32),
            pltpu.VMEM((heads, rows, 2 * HEAD_SIZE), F32),
            pltpu.VMEM((rows, q_width), BF16),
            pltpu.VMEM(out_weight.shape, BF16),
            pltpu.VMEM((inner - 1, OUTER * own, width), BF16),
            pltpu.VMEM((inner - 1, OUTER * own, width), BF16),
            pltpu.VMEM((OUTER, own, width), F32),
            pltpu.VMEM((own, width), BF16),
            pltpu.VMEM((own, width), BF16),
            dma,
            dma((sp_count,)),
            dma((sp_count,)),
            dma((sp_count,)),
            dma((sp_count,)),
            dma((inner - 1,)),
            dma((inner - 1,)),
            dma,
            dma,
        ],
        compiler_params=pltpu.CompilerParams(
            collective_id=0, has_side_effects=True, vmem_limit_bytes=40 * 2**20
        ),
        name="mix",
    )(
        queries,
        key_value_pairs,
        forget_gate_total,
        forget_gate_total.T,
        residual_in,
        norm_gain.reshape(1, -1),
        out_weight,
    )

    top = routes.shape[1]
    cap = max(2, 3 * own * top // (2 * sp_count))
    cap = -(-cap // 8) * 8
    flat = routes.reshape(-1)
    order = jnp.arange(flat.shape[0], dtype=jnp.int32)
    same = (flat[:, None] == flat[None, :]) & (order[None, :] < order[:, None])
    slot = (flat * cap + jnp.sum(same.astype(jnp.int32), axis=1)).reshape(own, top)
    ff = expert_gate.shape[2]
    block = (cap, width)
    return pl.pallas_call(
        functools.partial(expert_kernel, sp_count, tp_count, cap),
        out_shape=jax.ShapeDtypeStruct((own, width), BF16),
        in_specs=[vmem] * 5 + [hbm] * 3,
        out_specs=vmem,
        scratch_shapes=[
            pltpu.VMEM((sp_count,) + block, BF16),
            pltpu.VMEM((sp_count, inner, OUTER) + block, BF16),
            pltpu.VMEM((width, ff), BF16),
            pltpu.VMEM((width, ff), BF16),
            pltpu.VMEM((ff, width), BF16),
            pltpu.VMEM((sp_count, inner, OUTER) + block, BF16),
            pltpu.VMEM((inner - 1, sp_count, OUTER) + block, BF16),
            pltpu.VMEM((sp_count, OUTER) + block, BF16),
            pltpu.VMEM((sp_count,) + block, BF16),
            pltpu.VMEM((sp_count,) + block, BF16),
            pltpu.VMEM((sp_count,) + block, BF16),
            dma((3,)),
            dma,
            dma((sp_count,)),
            dma((sp_count,)),
            dma((sp_count,)),
            dma((sp_count,)),
            dma((inner - 1, sp_count)),
            dma((inner - 1, sp_count)),
            dma((inner - 1, sp_count)),
            dma((inner - 1, sp_count)),
            dma((inner - 1, sp_count)),
            dma((inner - 1, sp_count)),
            dma((sp_count,)),
            dma((sp_count,)),
            dma((sp_count,)),
            dma((sp_count,)),
        ],
        compiler_params=pltpu.CompilerParams(
            collective_id=1, has_side_effects=True, vmem_limit_bytes=60 * 2**20
        ),
        name="experts",
    )(normed, hidden, slot, slot.T, route_weight, expert_gate, expert_up, expert_down)


def solution(mesh):
    return jax.shard_map(
        local,
        mesh=mesh,
        in_specs=(
            P("sp", "tp"),
            P("sp", "tp"),
            P("sp", "tp"),
            P(("sp", "tp"), None),
            P("tp", None),
            P(),
            P(("sp", "tp"), None),
            P(("sp", "tp"), None),
            P("sp", None, "tp"),
            P("sp", None, "tp"),
            P("sp", "tp", None),
        ),
        out_specs=P(("sp", "tp"), None),
        check_vma=False,
    )
```

```python
import functools

import jax
import jax.numpy as jnp
from jax import lax
from jax.experimental import pallas as pl
from jax.experimental.pallas import tpu as pltpu
from jax.sharding import PartitionSpec as P

HEAD_SIZE = 64
NEG_FILL = -1e30
NORM_EPS = 1e-06
OUTER = 2
MESH = pl.DeviceIdType.MESH
F32 = jnp.float32
BF16 = jnp.bfloat16


def greet(peers_sp, sp_count, sp, tp, tp_peers):
    barrier = pltpu.get_barrier_semaphore()

    def signal(step, carry):
        pl.semaphore_signal(
            barrier, inc=1, device_id=(lax.rem(sp + step, sp_count), tp), device_id_type=MESH
        )
        return carry

    lax.fori_loop(1, sp_count, signal, 0)
    for peer in tp_peers:
        pl.semaphore_signal(barrier, inc=1, device_id=(sp, peer), device_id_type=MESH)
    return lambda: pl.semaphore_wait(barrier, sp_count - 1 + len(tp_peers))


def remote(src, dst, send, recv, device):
    return pltpu.make_async_remote_copy(
        src_ref=src,
        dst_ref=dst,
        send_sem=send,
        recv_sem=recv,
        device_id=device,
        device_id_type=MESH,
    )


def tp_places(tp, tp_count):
    inner = tp_count // OUTER
    a, c = tp // inner, lax.rem(tp, inner)
    mates = [a * inner + lax.rem(c + k, inner) for k in range(1, inner)]
    across = (1 - a) * inner + c
    return inner, a, c, mates, across


def layer_kernel(
    sp_count,
    tp_count,
    cap,
    q_hbm,
    kv_hbm,
    gates_hbm,
    resid_hbm,
    gain_hbm,
    wout_hbm,
    routes_hbm,
    weight_hbm,
    gate_hbm,
    up_hbm,
    down_hbm,
    out_ref,
    q_ref,
    kv_ref,
    gate_rows_ref,
    resid_ref,
    gain_ref,
    routes_ref,
    weight_ref,
    kv_all,
    gate_all,
    gate_ref,
    qm_ref,
    max_ref,
    acc_ref,
    att_ref,
    wout,
    mate_out,
    mate_back,
    own_sum,
    far_out,
    far_back,
    hidden_ref,
    outgoing,
    inbox,
    w_gate,
    w_up,
    w_down,
    partial,
    mate_in,
    chip_sum,
    far_in,
    final,
    back,
    in_sem,
    w_sem,
    kv_send,
    kv_recv,
    gate_send,
    gate_recv,
    mate_send,
    mate_recv,
    far_send,
    far_recv,
    own_sem,
    s1,
    r1,
    s2,
    r2,
    s3,
    r3,
    s4,
    r4,
    s5,
    r5,
    s6,
    r6,
    s7,
    r7,
):
    sp, tp = lax.axis_index("sp"), lax.axis_index("tp")
    inner, a, c, mates, across = tp_places(tp, tp_count)
    rows, q_width = q_ref.shape
    heads = q_width // HEAD_SIZE
    pair = 2 * HEAD_SIZE
    groups = kv_ref.shape[1] // pair
    per_group = heads // groups
    own = rows // tp_count
    ready = greet(None, sp_count, sp, tp, mates + [across])
    fetches = [
        pltpu.make_async_copy(src, dst, in_sem.at[i])
        for i, (src, dst) in enumerate(
            (
                (kv_hbm, kv_ref),
                (gates_hbm, gate_rows_ref),
                (q_hbm, q_ref),
                (routes_hbm, routes_ref),
                (weight_hbm, weight_ref),
                (resid_hbm, resid_ref),
                (gain_hbm, gain_ref),
                (wout_hbm, wout),
            )
        )
    ]
    for fetch in fetches:
        fetch.start()
    loads = [
        pltpu.make_async_copy(src.at[0], dst, w_sem.at[i])
        for i, (src, dst) in enumerate(
            ((gate_hbm, w_gate), (up_hbm, w_up), (down_hbm, w_down))
        )
    ]
    for load in loads:
        load.start()
    fetches[0].wait()
    fetches[1].wait()
    ready()


    def kv_copy(source, target):
        return remote(
            kv_ref, kv_all.at[source], kv_send.at[target], kv_recv.at[source], (target, tp)
        )

    def gate_copy(source, target):
        return remote(
            gate_rows_ref,
            gate_all.at[source],
            gate_send.at[target],
            gate_recv.at[source],
            (target, tp),
        )

    def send(target, carry):
        kv_copy(sp, target).start()
        gate_copy(sp, target).start()
        return carry

    lax.fori_loop(sp + 1, sp_count, send, 0)

    fetches[2].wait()
    gate_ref[...] = gate_rows_ref[...].T
    low = lax.broadcasted_iota(jnp.int32, (rows, pair), 1) < HEAD_SIZE
    for h in range(heads):
        base = (h // 2) * pair
        block = q_ref[:, base : base + pair].astype(F32) * (HEAD_SIZE**-0.5)
        keep = low if h % 2 == 0 else jnp.logical_not(low)
        qm_ref[h] = jnp.where(keep, block, 0.0).astype(BF16)

    def attend(kv, gates, first):
        causal = None
        if first:
            causal = lax.broadcasted_iota(jnp.int32, (rows, rows), 1) <= lax.broadcasted_iota(
                jnp.int32, (rows, rows), 0
            )
        for g in range(groups):
            both = kv[:, g * pair : (g + 1) * pair].astype(F32)
            swapped = pltpu.roll(both, HEAD_SIZE, 1)
            keys = jnp.where(low, both, swapped).astype(BF16)
            values = (
                jnp.where(low, swapped, 1.0).astype(BF16),
                jnp.where(low, 1.0, both).astype(BF16),
            )
            for h in range(g * per_group, (g + 1) * per_group):
                scores = lax.dot_general(
                    qm_ref[h], keys, (((1,), (1,)), ((), ())), preferred_element_type=F32
                )
                scores = scores + gate_ref[:, h : h + 1] - gates[h : h + 1, :]
                if first:
                    scores = jnp.where(causal, scores, NEG_FILL)
                top = jnp.max(scores, axis=1, keepdims=True)
                if not first:
                    old = max_ref[h]
                    top = jnp.maximum(old, top)
                weights = jnp.exp(scores - top).astype(BF16)
                block_sum = jnp.dot(weights, values[h % 2], preferred_element_type=F32)
                if first:
                    acc_ref[h] = block_sum
                else:
                    acc_ref[h] = acc_ref[h] * jnp.exp(old - top) + block_sum
                max_ref[h] = top

    attend(kv_ref[...], gate_rows_ref[...], True)

    def earlier(step, carry):
        source = sp - step
        kv_copy(source, sp).wait_recv()
        gate_copy(source, sp).wait_recv()
        attend(kv_all[source], gate_all[source], False)
        return carry

    lax.fori_loop(1, sp + 1, earlier, 0)

    for h in range(0, heads, 2):
        even, odd = acc_ref[h], acc_ref[h + 1]
        even = even / pltpu.roll(even, HEAD_SIZE, 1)
        odd = odd / pltpu.roll(odd, HEAD_SIZE, 1)
        att_ref[:, (h // 2) * pair : (h // 2 + 1) * pair] = jnp.where(low, even, odd).astype(BF16)

    for fetch in fetches[3:]:
        fetch.wait()

    def product(column):
        parts = [
            att_ref[pl.ds(pl.multiple_of((o * inner + column) * own, own), own), :]
            for o in range(OUTER)
        ]
        return jnp.dot(jnp.concatenate(parts, axis=0), wout[...], preferred_element_type=F32)

    mate_copies = []
    for k, mate in enumerate(mates):
        mate_out[k] = product(lax.rem(mate, inner)).astype(BF16)
        copy = remote(
            mate_out.at[k], mate_back.at[k], mate_send.at[k], mate_recv.at[k], (sp, mate)
        )
        copy.start()
        mate_copies.append(copy)
    own_sum[...] = product(c).reshape(OUTER, own, own_sum.shape[2])
    for k, copy in enumerate(mate_copies):
        copy.wait_recv()
        own_sum[...] += mate_back[k].astype(F32).reshape(own_sum.shape)
    far_out[...] = own_sum[1 - a].astype(BF16)
    far = remote(far_out, far_back, far_send, far_recv, (sp, across))
    far.start()
    far.wait_recv()
    hidden = resid_ref[...].astype(F32) + own_sum[a] + far_back[...].astype(F32)
    hidden_ref[...] = hidden
    scale = lax.rsqrt(jnp.mean(hidden * hidden, axis=1, keepdims=True) + NORM_EPS)
    normed = (hidden * scale * gain_ref[...]).astype(BF16)

    width = out_ref.shape[1]
    slots = sp_count * cap
    top_count = routes_ref.shape[0]
    expert_at = lax.broadcasted_iota(jnp.int32, (sp_count, own), 0)
    earlier_row = lax.broadcasted_iota(jnp.int32, (own, own), 0) < lax.broadcasted_iota(
        jnp.int32, (own, own), 1
    )
    ahead = jnp.where(earlier_row, 1.0, 0.0).astype(BF16)
    slot_at = lax.broadcasted_iota(jnp.int32, (slots, own), 0).astype(F32)
    first_slot = expert_at.astype(F32) * cap
    taken = jnp.zeros((sp_count, 1), F32)
    pick = jnp.zeros((slots, own), F32)
    share = jnp.zeros((slots, own), F32)
    for k in range(top_count):
        named = jnp.where(expert_at == routes_ref[k : k + 1, :], 1.0, 0.0)
        rank = jnp.dot(named.astype(BF16), ahead, preferred_element_type=F32)
        slot = jnp.sum(named * (first_slot + rank + taken), axis=0, keepdims=True)
        taken = taken + jnp.sum(named, axis=1, keepdims=True)
        hit = slot_at == slot
        pick = pick + jnp.where(hit, 1.0, 0.0)
        share = share + jnp.where(hit, weight_ref[k : k + 1, :], 0.0)
    sent = jnp.dot(pick.astype(BF16), normed, preferred_element_type=F32)
    outgoing[...] = sent.reshape(sp_count, cap, width).astype(BF16)

    def at(step):
        return lax.rem(sp + step, sp_count)

    def before(step):
        return lax.rem(sp + sp_count - step, sp_count)

    def to_expert(target, source):
        return remote(
            outgoing.at[target], inbox.at[source, c, a], s1.at[target], r1.at[source], (target, tp)
        )

    def to_across(source):
        return remote(
            inbox.at[source, c, a], inbox.at[source, c, a], s2.at[source], r2.at[source], (sp, across)
        )

    def from_across(source):
        return remote(
            inbox.at[source, c, a],
            inbox.at[source, c, 1 - a],
            s2.at[source],
            r2.at[source],
            (sp, across),
        )

    def to_mate(k, source, o, send, recv):
        return remote(
            inbox.at[source, c, o], inbox.at[source, c, o], send.at[k, source], recv.at[k, source],
            (sp, mates[k]),
        )

    def from_mate(k, source, o, send, recv):
        sender = lax.rem(c + inner - (k + 1), inner)
        return remote(
            inbox.at[source, c, o],
            inbox.at[source, sender, o],
            send.at[k, source],
            recv.at[k, source],
            (sp, mates[k]),
        )

    def start_one(step, carry):
        to_expert(before(step), sp).start()
        return carry

    lax.fori_loop(1, sp_count, start_one, 0)
    keep = pltpu.make_async_copy(outgoing.at[sp], inbox.at[sp, c, a], own_sem)
    keep.start()
    keep.wait()

    def forward(source):
        to_across(source).start()
        for k in range(len(mates)):
            to_mate(k, source, a, s3, r3).start()

    def forward_across(source):
        from_across(source).wait_recv()
        for k in range(len(mates)):
            to_mate(k, source, 1 - a, s4, r4).start()

    def accept(step):
        source = at(step)

        @pl.when(step > 0)
        def _():
            to_expert(sp, source).wait_recv()

        forward(source)

    def arrived(step):
        source = at(step)
        for k in range(len(mates)):
            from_mate(k, source, a, s3, r3).wait_recv()
            from_mate(k, source, 1 - a, s4, r4).wait_recv()

    def load_rows(source):
        return inbox[source].astype(F32).reshape(tp_count * cap, width).astype(BF16)

    def send_mate(k, source):
        return remote(
            partial.at[source, lax.rem(mates[k], inner)],
            mate_in.at[k, source],
            s5.at[k, source],
            r5.at[k, source],
            (sp, mates[k]),
        )

    def send_far(source):
        return remote(
            chip_sum.at[source, 1 - a], far_in.at[source], s6.at[source], r6.at[source], (sp, across)
        )

    def send_back(target, source):
        return remote(
            final.at[target], back.at[source], s7.at[target], r7.at[source], (target, tp)
        )

    batch = 2 if sp_count % 2 == 0 else 1
    steps = sp_count // batch

    def ffn(i):
        for b in range(batch):
            arrived(i * batch + b)
        x = jnp.concatenate([load_rows(at(i * batch + b)) for b in range(batch)], axis=0)
        gate = jnp.dot(x, w_gate[...], preferred_element_type=F32)
        up = jnp.dot(x, w_up[...], preferred_element_type=F32)
        hidden = (gate / (1.0 + jnp.exp(-gate)) * up).astype(BF16)
        y = jnp.dot(hidden, w_down[...], preferred_element_type=F32)
        y = y.reshape(batch, inner, OUTER, cap, width).astype(BF16)
        for b in range(batch):
            source = at(i * batch + b)
            partial[source] = y[b]
            for k in range(len(mates)):
                send_mate(k, source).start()

    def chip(i):
        for b in range(batch):
            source = at(i * batch + b)
            total = partial[source, c].astype(F32)
            for k in range(len(mates)):
                send_mate(k, source).wait_recv()
                total = total + mate_in[k, source].astype(F32)
            chip_sum[source] = total.astype(BF16)
            send_far(source).start()

    def give_back(i):
        for b in range(batch):
            step = i * batch + b
            source = at(step)
            send_far(source).wait_recv()
            total = chip_sum[source, a].astype(F32) + far_in[source].astype(F32)
            final[source] = total.astype(BF16)

            @pl.when(step > 0)
            def _():
                send_back(source, sp).start()

    def pipeline(i, carry):
        @pl.when(i + 1 < steps)
        def _():
            for b in range(batch):
                accept((i + 1) * batch + b)

        for b in range(batch):
            forward_across(at(i * batch + b))
        ffn(i)

        @pl.when(i >= 1)
        def _():
            chip(i - 1)

        @pl.when(i >= 2)
        def _():
            give_back(i - 2)

        return carry

    for b in range(batch):
        accept(b)
    for load in loads:
        load.wait()
    lax.fori_loop(0, steps, pipeline, 0)
    chip(steps - 1)
    if steps >= 2:
        give_back(steps - 2)
    give_back(steps - 1)
    back[sp] = final[sp]

    high = share.astype(BF16)
    rest = share - high.astype(F32)
    middle = rest.astype(BF16)
    least = (rest - middle.astype(F32)).astype(BF16)

    def arrive(step, carry):
        send_back(sp, at(step)).wait_recv()
        return carry

    lax.fori_loop(1, sp_count, arrive, 0)
    results = back[...].astype(F32).reshape(slots, width).astype(BF16)
    combined = hidden_ref[...]
    for piece in (high, middle, least):
        combined = combined + lax.dot_general(
            piece, results, (((0,), (0,)), ((), ())), preferred_element_type=F32
        )
    out_ref[...] = combined.astype(BF16)

    def finish(step, carry):
        source = at(step)
        to_across(source).wait_send()
        send_far(source).wait_send()
        for k in range(len(mates)):
            to_mate(k, source, a, s3, r3).wait_send()
            to_mate(k, source, 1 - a, s4, r4).wait_send()
            send_mate(k, source).wait_send()

        @pl.when(step > 0)
        def _():
            to_expert(source, sp).wait_send()
            send_back(source, sp).wait_send()

        return carry

    lax.fori_loop(0, sp_count, finish, 0)
    far.wait_send()
    for copy in mate_copies:
        copy.wait_send()

    def finish_mix(target, carry):
        kv_copy(sp, target).wait_send()
        gate_copy(sp, target).wait_send()
        return carry

    lax.fori_loop(sp + 1, sp_count, finish_mix, 0)


def local(
    queries,
    key_value_pairs,
    forget_gate_total,
    residual_in,
    out_weight,
    norm_gain,
    routes,
    route_weight,
    expert_gate,
    expert_up,
    expert_down,
):
    sp_count = lax.axis_size("sp")
    tp_count = lax.axis_size("tp")
    rows, q_width = queries.shape
    heads = q_width // HEAD_SIZE
    own, width = residual_in.shape
    inner = tp_count // OUTER
    top = routes.shape[1]
    cap = max(2, 3 * own * top // (2 * sp_count))
    cap = -(-cap // 8) * 8
    ff = expert_gate.shape[2]
    block = (cap, width)
    dma = pltpu.SemaphoreType.DMA
    some, mate = dma((sp_count,)), dma((inner - 1, sp_count))
    hbm = pl.BlockSpec(memory_space=pl.ANY)
    return pl.pallas_call(
        functools.partial(layer_kernel, sp_count, tp_count, cap),
        out_shape=jax.ShapeDtypeStruct((own, width), BF16),
        in_specs=[hbm] * 11,
        out_specs=pl.BlockSpec(memory_space=pltpu.VMEM),
        scratch_shapes=[
            pltpu.VMEM(queries.shape, BF16),
            pltpu.VMEM(key_value_pairs.shape, BF16),
            pltpu.VMEM((heads, rows), F32),
            pltpu.VMEM((own, width), BF16),
            pltpu.VMEM((1, width), F32),
            pltpu.VMEM((top, own), jnp.int32),
            pltpu.VMEM((top, own), F32),
            pltpu.VMEM((sp_count, rows, key_value_pairs.shape[1]), BF16),
            pltpu.VMEM((sp_count, heads, rows), F32),
            pltpu.VMEM((rows, heads), F32),
            pltpu.VMEM((heads, rows, 2 * HEAD_SIZE), BF16),
            pltpu.VMEM((heads, rows, 1), F32),
            pltpu.VMEM((heads, rows, 2 * HEAD_SIZE), F32),
            pltpu.VMEM((rows, q_width), BF16),
            pltpu.VMEM(out_weight.shape, BF16),
            pltpu.VMEM((inner - 1, OUTER * own, width), BF16),
            pltpu.VMEM((inner - 1, OUTER * own, width), BF16),
            pltpu.VMEM((OUTER, own, width), F32),
            pltpu.VMEM((own, width), BF16),
            pltpu.VMEM((own, width), BF16),
            pltpu.VMEM((own, width), F32),
            pltpu.VMEM((sp_count,) + block, BF16),
            pltpu.VMEM((sp_count, inner, OUTER) + block, BF16),
            pltpu.VMEM((width, ff), BF16),
            pltpu.VMEM((width, ff), BF16),
            pltpu.VMEM((ff, width), BF16),
            pltpu.VMEM((sp_count, inner, OUTER) + block, BF16),
            pltpu.VMEM((inner - 1, sp_count, OUTER) + block, BF16),
            pltpu.VMEM((sp_count, OUTER) + block, BF16),
            pltpu.VMEM((sp_count,) + block, BF16),
            pltpu.VMEM((sp_count,) + block, BF16),
            pltpu.VMEM((sp_count,) + block, BF16),
            dma((8,)),
            dma((3,)),
            some,
            some,
            some,
            some,
            dma((inner - 1,)),
            dma((inner - 1,)),
            dma,
            dma,
            dma,
        ]
        + [some] * 4
        + [mate] * 6
        + [some] * 4,
        compiler_params=pltpu.CompilerParams(
            collective_id=0, has_side_effects=True, vmem_limit_bytes=63 * 2**20
        ),
        name="layer",
    )(
        queries,
        key_value_pairs,
        forget_gate_total.T,
        residual_in,
        norm_gain.reshape(1, -1),
        out_weight,
        routes.T,
        route_weight.T,
        expert_gate,
        expert_up,
        expert_down,
    )


def solution(mesh):
    return jax.shard_map(
        local,
        mesh=mesh,
        in_specs=(
            P("sp", "tp"),
            P("sp", "tp"),
            P("sp", "tp"),
            P(("sp", "tp"), None),
            P("tp", None),
            P(),
            P(("sp", "tp"), None),
            P(("sp", "tp"), None),
            P("sp", None, "tp"),
            P("sp", None, "tp"),
            P("sp", "tp", None),
        ),
        out_specs=P(("sp", "tp"), None),
        check_vma=False,
    )
```

```python
import functools

import jax
import jax.numpy as jnp
from jax import lax
from jax.experimental import pallas as pl
from jax.experimental.pallas import tpu as pltpu
from jax.sharding import PartitionSpec as P

HEAD_SIZE = 64
NEG_FILL = -1e30
NORM_EPS = 1e-06
OUTER = 2
MESH = pl.DeviceIdType.MESH
F32 = jnp.float32
BF16 = jnp.bfloat16


def greet(peers_sp, sp_count, sp, tp, tp_peers):
    barrier = pltpu.get_barrier_semaphore()

    def signal(step, carry):
        pl.semaphore_signal(
            barrier, inc=1, device_id=(lax.rem(sp + step, sp_count), tp), device_id_type=MESH
        )
        return carry

    lax.fori_loop(1, sp_count, signal, 0)
    for peer in tp_peers:
        pl.semaphore_signal(barrier, inc=1, device_id=(sp, peer), device_id_type=MESH)
    return lambda: pl.semaphore_wait(barrier, sp_count - 1 + len(tp_peers))


def remote(src, dst, send, recv, device):
    return pltpu.make_async_remote_copy(
        src_ref=src,
        dst_ref=dst,
        send_sem=send,
        recv_sem=recv,
        device_id=device,
        device_id_type=MESH,
    )


def tp_places(tp, tp_count):
    inner = tp_count // OUTER
    a, c = tp // inner, lax.rem(tp, inner)
    mates = [a * inner + lax.rem(c + k, inner) for k in range(1, inner)]
    across = (1 - a) * inner + c
    return inner, a, c, mates, across


def layer_kernel(
    sp_count,
    tp_count,
    cap,
    q_hbm,
    kv_hbm,
    gates_hbm,
    resid_hbm,
    gain_hbm,
    wout_hbm,
    routes_hbm,
    weight_hbm,
    gate_hbm,
    up_hbm,
    down_hbm,
    out_ref,
    q_ref,
    kv_ref,
    gate_rows_ref,
    resid_ref,
    gain_ref,
    routes_ref,
    weight_ref,
    kv_all,
    gate_all,
    gate_ref,
    qm_ref,
    max_ref,
    acc_ref,
    att_ref,
    wout,
    mate_out,
    mate_back,
    own_sum,
    far_out,
    far_back,
    hidden_ref,
    outgoing,
    inbox,
    w_gate,
    w_up,
    w_down,
    partial,
    mate_in,
    chip_sum,
    far_in,
    final,
    back,
    in_sem,
    w_sem,
    kv_send,
    kv_recv,
    gate_send,
    gate_recv,
    mate_send,
    mate_recv,
    far_send,
    far_recv,
    own_sem,
    s1,
    r1,
    s2,
    r2,
    s3,
    r3,
    s4,
    r4,
    s5,
    r5,
    s6,
    r6,
    s7,
    r7,
):
    sp, tp = lax.axis_index("sp"), lax.axis_index("tp")
    inner, a, c, mates, across = tp_places(tp, tp_count)
    rows, q_width = q_ref.shape
    heads = q_width // HEAD_SIZE
    pair = 2 * HEAD_SIZE
    groups = kv_ref.shape[1] // pair
    per_group = heads // groups
    own = rows // tp_count
    ready = greet(None, sp_count, sp, tp, mates + [across])
    fetches = [
        pltpu.make_async_copy(src, dst, in_sem.at[i])
        for i, (src, dst) in enumerate(
            (
                (kv_hbm, kv_ref),
                (gates_hbm, gate_rows_ref),
                (q_hbm, q_ref),
                (routes_hbm, routes_ref),
                (weight_hbm, weight_ref),
                (resid_hbm, resid_ref),
                (gain_hbm, gain_ref),
                (wout_hbm, wout),
            )
        )
    ]
    for fetch in fetches:
        fetch.start()
    loads = [
        pltpu.make_async_copy(src.at[0], dst, w_sem.at[i])
        for i, (src, dst) in enumerate(
            ((gate_hbm, w_gate), (up_hbm, w_up), (down_hbm, w_down))
        )
    ]
    for load in loads:
        load.start()
    fetches[0].wait()
    fetches[1].wait()
    ready()


    def kv_copy(source, target):
        return remote(
            kv_ref, kv_all.at[source], kv_send.at[target], kv_recv.at[source], (target, tp)
        )

    def gate_copy(source, target):
        return remote(
            gate_rows_ref,
            gate_all.at[source],
            gate_send.at[target],
            gate_recv.at[source],
            (target, tp),
        )

    def send(target, carry):
        kv_copy(sp, target).start()
        gate_copy(sp, target).start()
        return carry

    lax.fori_loop(sp + 1, sp_count, send, 0)

    fetches[2].wait()
    gate_ref[...] = gate_rows_ref[...].T
    low = lax.broadcasted_iota(jnp.int32, (rows, pair), 1) < HEAD_SIZE
    for h in range(heads):
        base = (h // 2) * pair
        block = q_ref[:, base : base + pair].astype(F32) * (HEAD_SIZE**-0.5)
        keep = low if h % 2 == 0 else jnp.logical_not(low)
        qm_ref[h] = jnp.where(keep, block, 0.0).astype(BF16)

    def attend(kv, gates, first):
        causal = None
        if first:
            causal = lax.broadcasted_iota(jnp.int32, (rows, rows), 1) <= lax.broadcasted_iota(
                jnp.int32, (rows, rows), 0
            )
        for g in range(groups):
            both = kv[:, g * pair : (g + 1) * pair].astype(F32)
            swapped = pltpu.roll(both, HEAD_SIZE, 1)
            keys = jnp.where(low, both, swapped).astype(BF16)
            values = (
                jnp.where(low, swapped, 1.0).astype(BF16),
                jnp.where(low, 1.0, both).astype(BF16),
            )
            for h in range(g * per_group, (g + 1) * per_group):
                scores = lax.dot_general(
                    qm_ref[h], keys, (((1,), (1,)), ((), ())), preferred_element_type=F32
                )
                scores = scores + gate_ref[:, h : h + 1] - gates[h : h + 1, :]
                if first:
                    scores = jnp.where(causal, scores, NEG_FILL)
                top = jnp.max(scores, axis=1, keepdims=True)
                if not first:
                    old = max_ref[h]
                    top = jnp.maximum(old, top)
                weights = jnp.exp(scores - top).astype(BF16)
                block_sum = jnp.dot(weights, values[h % 2], preferred_element_type=F32)
                if first:
                    acc_ref[h] = block_sum
                else:
                    acc_ref[h] = acc_ref[h] * jnp.exp(old - top) + block_sum
                max_ref[h] = top

    attend(kv_ref[...], gate_rows_ref[...], True)

    def earlier(step, carry):
        source = sp - step
        kv_copy(source, sp).wait_recv()
        gate_copy(source, sp).wait_recv()
        attend(kv_all[source], gate_all[source], False)
        return carry

    lax.fori_loop(1, sp + 1, earlier, 0)

    for h in range(0, heads, 2):
        even, odd = acc_ref[h], acc_ref[h + 1]
        even = even / pltpu.roll(even, HEAD_SIZE, 1)
        odd = odd / pltpu.roll(odd, HEAD_SIZE, 1)
        att_ref[:, (h // 2) * pair : (h // 2 + 1) * pair] = jnp.where(low, even, odd).astype(BF16)

    for fetch in fetches[3:]:
        fetch.wait()

    def product(column):
        parts = [
            att_ref[pl.ds(pl.multiple_of((o * inner + column) * own, own), own), :]
            for o in range(OUTER)
        ]
        return jnp.dot(jnp.concatenate(parts, axis=0), wout[...], preferred_element_type=F32)

    mate_copies = []
    for k, mate in enumerate(mates):
        mate_out[k] = product(lax.rem(mate, inner)).astype(BF16)
        copy = remote(
            mate_out.at[k], mate_back.at[k], mate_send.at[k], mate_recv.at[k], (sp, mate)
        )
        copy.start()
        mate_copies.append(copy)
    own_sum[...] = product(c).reshape(OUTER, own, own_sum.shape[2])
    for k, copy in enumerate(mate_copies):
        copy.wait_recv()
        own_sum[...] += mate_back[k].astype(F32).reshape(own_sum.shape)
    far_out[...] = own_sum[1 - a].astype(BF16)
    far = remote(far_out, far_back, far_send, far_recv, (sp, across))
    far.start()
    far.wait_recv()
    hidden = resid_ref[...].astype(F32) + own_sum[a] + far_back[...].astype(F32)
    hidden_ref[...] = hidden
    scale = lax.rsqrt(jnp.mean(hidden * hidden, axis=1, keepdims=True) + NORM_EPS)
    normed = (hidden * scale * gain_ref[...]).astype(BF16)

    width = out_ref.shape[1]
    slots = sp_count * cap
    top_count = routes_ref.shape[0]
    expert_at = lax.broadcasted_iota(jnp.int32, (sp_count, own), 0)
    earlier_row = lax.broadcasted_iota(jnp.int32, (own, own), 0) < lax.broadcasted_iota(
        jnp.int32, (own, own), 1
    )
    ahead = jnp.where(earlier_row, 1.0, 0.0).astype(BF16)
    slot_at = lax.broadcasted_iota(jnp.int32, (slots, own), 0).astype(F32)
    first_slot = expert_at.astype(F32) * cap
    taken = jnp.zeros((sp_count, 1), F32)
    pick = jnp.zeros((slots, own), F32)
    share = jnp.zeros((slots, own), F32)
    for k in range(top_count):
        named = jnp.where(expert_at == routes_ref[k : k + 1, :], 1.0, 0.0)
        rank = jnp.dot(named.astype(BF16), ahead, preferred_element_type=F32)
        slot = jnp.sum(named * (first_slot + rank + taken), axis=0, keepdims=True)
        taken = taken + jnp.sum(named, axis=1, keepdims=True)
        hit = slot_at == slot
        pick = pick + jnp.where(hit, 1.0, 0.0)
        share = share + jnp.where(hit, weight_ref[k : k + 1, :], 0.0)
    sent = jnp.dot(pick.astype(BF16), normed, preferred_element_type=F32)
    outgoing[...] = sent.reshape(sp_count, cap, width).astype(BF16)

    def at(step):
        return lax.rem(sp + step, sp_count)

    def before(step):
        return lax.rem(sp + sp_count - step, sp_count)

    def to_expert(target, source):
        return remote(
            outgoing.at[target], inbox.at[source, c, a], s1.at[target], r1.at[source], (target, tp)
        )

    def to_across(source):
        return remote(
            inbox.at[source, c, a], inbox.at[source, c, a], s2.at[source], r2.at[source], (sp, across)
        )

    def from_across(source):
        return remote(
            inbox.at[source, c, a],
            inbox.at[source, c, 1 - a],
            s2.at[source],
            r2.at[source],
            (sp, across),
        )

    def to_mate(k, source, o, send, recv):
        return remote(
            inbox.at[source, c, o], inbox.at[source, c, o], send.at[k, source], recv.at[k, source],
            (sp, mates[k]),
        )

    def from_mate(k, source, o, send, recv):
        sender = lax.rem(c + inner - (k + 1), inner)
        return remote(
            inbox.at[source, c, o],
            inbox.at[source, sender, o],
            send.at[k, source],
            recv.at[k, source],
            (sp, mates[k]),
        )

    def start_one(step, carry):
        to_expert(before(step), sp).start()
        return carry

    lax.fori_loop(1, sp_count, start_one, 0)
    keep = pltpu.make_async_copy(outgoing.at[sp], inbox.at[sp, c, a], own_sem)
    keep.start()
    keep.wait()

    def forward(source):
        to_across(source).start()
        for k in range(len(mates)):
            to_mate(k, source, a, s3, r3).start()

    def forward_across(source):
        from_across(source).wait_recv()
        for k in range(len(mates)):
            to_mate(k, source, 1 - a, s4, r4).start()

    def accept(step):
        source = at(step)

        @pl.when(step > 0)
        def _():
            to_expert(sp, source).wait_recv()

        forward(source)

    def arrived(step):
        source = at(step)
        for k in range(len(mates)):
            from_mate(k, source, a, s3, r3).wait_recv()
            from_mate(k, source, 1 - a, s4, r4).wait_recv()

    def load_rows(source):
        return inbox[source].astype(F32).reshape(tp_count * cap, width).astype(BF16)

    def send_mate(k, source):
        return remote(
            partial.at[source, lax.rem(mates[k], inner)],
            mate_in.at[k, source],
            s5.at[k, source],
            r5.at[k, source],
            (sp, mates[k]),
        )

    def send_far(source):
        return remote(
            chip_sum.at[source, 1 - a], far_in.at[source], s6.at[source], r6.at[source], (sp, across)
        )

    def send_back(target, source):
        return remote(
            final.at[target], back.at[source], s7.at[target], r7.at[source], (target, tp)
        )

    batch = 2 if sp_count % 2 == 0 else 1
    steps = sp_count // batch

    def ffn(i):
        for b in range(batch):
            arrived(i * batch + b)
        x = jnp.concatenate([load_rows(at(i * batch + b)) for b in range(batch)], axis=0)
        gate = jnp.dot(x, w_gate[...], preferred_element_type=F32)
        up = jnp.dot(x, w_up[...], preferred_element_type=F32)
        hidden = (gate / (1.0 + jnp.exp(-gate)) * up).astype(BF16)
        y = jnp.dot(hidden, w_down[...], preferred_element_type=F32)
        y = y.reshape(batch, inner, OUTER, cap, width).astype(BF16)
        for b in range(batch):
            source = at(i * batch + b)
            partial[source] = y[b]
            for k in range(len(mates)):
                send_mate(k, source).start()

    def chip(i):
        for b in range(batch):
            source = at(i * batch + b)
            total = partial[source, c].astype(F32)
            for k in range(len(mates)):
                send_mate(k, source).wait_recv()
                total = total + mate_in[k, source].astype(F32)
            chip_sum[source] = total.astype(BF16)
            send_far(source).start()

    def give_back(i):
        for b in range(batch):
            step = i * batch + b
            source = at(step)
            send_far(source).wait_recv()
            total = chip_sum[source, a].astype(F32) + far_in[source].astype(F32)
            final[source] = total.astype(BF16)

            @pl.when(step > 0)
            def _():
                send_back(source, sp).start()

    ahead_by = min(2, steps)

    def pipeline(i, carry):
        @pl.when(i + ahead_by < steps)
        def _():
            for b in range(batch):
                accept((i + ahead_by) * batch + b)

        for b in range(batch):
            forward_across(at(i * batch + b))

        @pl.when(i >= 1)
        def _():
            chip(i - 1)

        ffn(i)

        @pl.when(i >= 1)
        def _():
            give_back(i - 1)

        return carry

    for step in range(ahead_by * batch):
        accept(step)
    for load in loads:
        load.wait()
    lax.fori_loop(0, steps, pipeline, 0)
    chip(steps - 1)
    give_back(steps - 1)
    back[sp] = final[sp]

    high = share.astype(BF16)
    rest = share - high.astype(F32)
    middle = rest.astype(BF16)
    least = (rest - middle.astype(F32)).astype(BF16)

    def arrive(step, carry):
        send_back(sp, at(step)).wait_recv()
        return carry

    lax.fori_loop(1, sp_count, arrive, 0)
    results = back[...].astype(F32).reshape(slots, width).astype(BF16)
    combined = hidden_ref[...]
    for piece in (high, middle, least):
        combined = combined + lax.dot_general(
            piece, results, (((0,), (0,)), ((), ())), preferred_element_type=F32
        )
    out_ref[...] = combined.astype(BF16)

    def finish(step, carry):
        source = at(step)
        to_across(source).wait_send()
        send_far(source).wait_send()
        for k in range(len(mates)):
            to_mate(k, source, a, s3, r3).wait_send()
            to_mate(k, source, 1 - a, s4, r4).wait_send()
            send_mate(k, source).wait_send()

        @pl.when(step > 0)
        def _():
            to_expert(source, sp).wait_send()
            send_back(source, sp).wait_send()

        return carry

    lax.fori_loop(0, sp_count, finish, 0)
    far.wait_send()
    for copy in mate_copies:
        copy.wait_send()

    def finish_mix(target, carry):
        kv_copy(sp, target).wait_send()
        gate_copy(sp, target).wait_send()
        return carry

    lax.fori_loop(sp + 1, sp_count, finish_mix, 0)


def local(
    queries,
    key_value_pairs,
    forget_gate_total,
    residual_in,
    out_weight,
    norm_gain,
    routes,
    route_weight,
    expert_gate,
    expert_up,
    expert_down,
):
    sp_count = lax.axis_size("sp")
    tp_count = lax.axis_size("tp")
    rows, q_width = queries.shape
    heads = q_width // HEAD_SIZE
    own, width = residual_in.shape
    inner = tp_count // OUTER
    top = routes.shape[1]
    cap = max(2, 3 * own * top // (2 * sp_count))
    cap = -(-cap // 8) * 8
    ff = expert_gate.shape[2]
    block = (cap, width)
    dma = pltpu.SemaphoreType.DMA
    some, mate = dma((sp_count,)), dma((inner - 1, sp_count))
    hbm = pl.BlockSpec(memory_space=pl.ANY)
    return pl.pallas_call(
        functools.partial(layer_kernel, sp_count, tp_count, cap),
        out_shape=jax.ShapeDtypeStruct((own, width), BF16),
        in_specs=[hbm] * 11,
        out_specs=pl.BlockSpec(memory_space=pltpu.VMEM),
        scratch_shapes=[
            pltpu.VMEM(queries.shape, BF16),
            pltpu.VMEM(key_value_pairs.shape, BF16),
            pltpu.VMEM((heads, rows), F32),
            pltpu.VMEM((own, width), BF16),
            pltpu.VMEM((1, width), F32),
            pltpu.VMEM((top, own), jnp.int32),
            pltpu.VMEM((top, own), F32),
            pltpu.VMEM((sp_count, rows, key_value_pairs.shape[1]), BF16),
            pltpu.VMEM((sp_count, heads, rows), F32),
            pltpu.VMEM((rows, heads), F32),
            pltpu.VMEM((heads, rows, 2 * HEAD_SIZE), BF16),
            pltpu.VMEM((heads, rows, 1), F32),
            pltpu.VMEM((heads, rows, 2 * HEAD_SIZE), F32),
            pltpu.VMEM((rows, q_width), BF16),
            pltpu.VMEM(out_weight.shape, BF16),
            pltpu.VMEM((inner - 1, OUTER * own, width), BF16),
            pltpu.VMEM((inner - 1, OUTER * own, width), BF16),
            pltpu.VMEM((OUTER, own, width), F32),
            pltpu.VMEM((own, width), BF16),
            pltpu.VMEM((own, width), BF16),
            pltpu.VMEM((own, width), F32),
            pltpu.VMEM((sp_count,) + block, BF16),
            pltpu.VMEM((sp_count, inner, OUTER) + block, BF16),
            pltpu.VMEM((width, ff), BF16),
            pltpu.VMEM((width, ff), BF16),
            pltpu.VMEM((ff, width), BF16),
            pltpu.VMEM((sp_count, inner, OUTER) + block, BF16),
            pltpu.VMEM((inner - 1, sp_count, OUTER) + block, BF16),
            pltpu.VMEM((sp_count, OUTER) + block, BF16),
            pltpu.VMEM((sp_count,) + block, BF16),
            pltpu.VMEM((sp_count,) + block, BF16),
            pltpu.VMEM((sp_count,) + block, BF16),
            dma((8,)),
            dma((3,)),
            some,
            some,
            some,
            some,
            dma((inner - 1,)),
            dma((inner - 1,)),
            dma,
            dma,
            dma,
        ]
        + [some] * 4
        + [mate] * 6
        + [some] * 4,
        compiler_params=pltpu.CompilerParams(
            collective_id=0, has_side_effects=True, vmem_limit_bytes=63 * 2**20
        ),
        name="layer",
    )(
        queries,
        key_value_pairs,
        forget_gate_total.T,
        residual_in,
        norm_gain.reshape(1, -1),
        out_weight,
        routes.T,
        route_weight.T,
        expert_gate,
        expert_up,
        expert_down,
    )


def solution(mesh):
    return jax.shard_map(
        local,
        mesh=mesh,
        in_specs=(
            P("sp", "tp"),
            P("sp", "tp"),
            P("sp", "tp"),
            P(("sp", "tp"), None),
            P("tp", None),
            P(),
            P(("sp", "tp"), None),
            P(("sp", "tp"), None),
            P("sp", None, "tp"),
            P("sp", None, "tp"),
            P("sp", "tp", None),
        ),
        out_specs=P(("sp", "tp"), None),
        check_vma=False,
    )
```
